32 devices in a mesh: sp: 8 (over z, y), tp: 4 (over x, core).
Axes of the slice: x: 2, y: 2, z: 4, core: 2. Of those that a mesh axis runs over, the one named last changes fastest.
Arguments:
- latents: bfloat16 [2560, 2048], P(('sp', 'tp')), may hold values from -12.5 to 12.5, as said below
- context: bfloat16 [1024, 2048], P('sp'), may hold values from -120 to 120, as said below
- cond_vec: float32 [2048], replicated, may hold values from -6 to 6
- ctx_vec: float32 [2048], replicated, may hold values from -6 to 6
- shift_w: bfloat16 [2048, 2048], P('sp', 'tp'), may hold values from -0.125 to 0.125
- scale_w: bfloat16 [2048, 2048], P('sp', 'tp'), may hold values from -0.125 to 0.125
- modgate_w: bfloat16 [2048, 2048], P('sp', 'tp'), may hold values from -0.125 to 0.125
- query_down_weight: bfloat16 [2048, 512], replicated, may hold values from -0.125 to 0.125
- latent_down_weight: bfloat16 [2048, 256], replicated, may hold values from -0.125 to 0.125
- rot_down: bfloat16 [2048, 32], replicated, may hold values from -0.125 to 0.125
- gate_w: bfloat16 [2048, 2048], P(None, 'tp'), may hold values from -0.125 to 0.125
- query_norm_gain: float32 [512], replicated, may hold values from 0.1 to 1.9
- latent_norm_gain: float32 [256], replicated, may hold values from 0.1 to 1.9
- query_plain_weight: bfloat16 [512, 2048], P(None, 'tp'), may hold values from -0.25 to 0.25
- query_rotary_weight: bfloat16 [512, 1024], P(None, 'tp'), may hold values from -0.25 to 0.25
- key_expand_weight: bfloat16 [256, 2048], P(None, 'tp'), may hold values from -0.375 to 0.375
- value_expand_weight: bfloat16 [256, 2048], P(None, 'tp'), may hold values from -0.375 to 0.375
- out_w: bfloat16 [2048, 2048], P('tp'), may hold values from -0.5 to 0.5
- norm_gain: float32 [2048], replicated, may hold values from 0.1 to 1.9
- norm_bias: float32 [2048], replicated, may hold values from -3 to 3
Outputs:
- mixed_out: bfloat16 [2560, 2048], P(('sp', 'tp'))
The draws below stay inside these ranges and needn't reach their ends.
Inputs may be any that keep to these rules, and one draw needn't show every extreme that they name: `latents`: latent rows are noise plus three slow waves along the whole sequence. Most context rows have their own scales of 1 to 3; a few rows may be far larger.
All inputs are finite; a program needn't handle non-finite values.
Results may differ from the reference program's by a relative error of at most 0.024.
The reference program's roundings to bfloat16 on the way count: a program that leaves them out, or rounds other values in their place, can miss the bound.
Values may be sent and summed in bfloat16 or wider, within the bound.
A program may use at most 128 MiB of HBM per device.

```python
import math
import jax
import jax.numpy as jnp
from jax import lax

MODEL_WIDTH = 2048
HEAD_COUNT = 32
QUERY_LATENT = 512
LATENT_WIDTH = 256
PLAIN_HEAD_SIZE = 64
ROTARY_SIZE = 32
VALUE_HEAD_SIZE = 64
GRID_W = 64
TOK_DEV = 320
CTX = 1024
TOKENS = 2560
N_TP = 4


def draw_latents(key, part):
    noise_key, wave_key, phase_key = jax.random.split(key, 3)
    noise_part = jnp.clip(jax.random.normal(noise_key, (TOKENS, MODEL_WIDTH), jnp.float32), -5.0, 5.0)
    directions = jnp.clip(jax.random.normal(wave_key, (3, MODEL_WIDTH), jnp.float32), -2.5, 2.5)
    phases = jax.random.uniform(phase_key, (3,), jnp.float32, 0.0, 2.0 * math.pi)
    position = jnp.arange(TOKENS, dtype=jnp.float32) / TOKENS
    frequency = jnp.arange(1, 4, dtype=jnp.float32)
    wave_part = jnp.cos(2.0 * math.pi * position[:, None] * frequency[None, :] + phases[None, :])
    return (noise_part + wave_part @ directions).astype(jnp.bfloat16)


def draw_context(key, part):
    value_key, scale_key, pick_key, large_key = jax.random.split(key, 4)
    row_scale = jnp.exp(jax.random.uniform(scale_key, (CTX, 1), jnp.float32, 0.0, math.log(3.0)))
    values = jnp.clip(jax.random.normal(value_key, (CTX, MODEL_WIDTH), jnp.float32), -6.0, 6.0) * row_scale
    return values.astype(jnp.bfloat16)


def level_of(own_key, shape, cuts, smallest, largest):
    loudness, own = 1.0, jax.random.fold_in(own_key, 6)
    for dim, blocks in cuts:
        heights = jnp.exp(jax.random.uniform(jax.random.fold_in(own, dim), (blocks,), jnp.float32, smallest / len(cuts), largest / len(cuts)))
        loudness = loudness * jnp.repeat(heights, shape[dim] // blocks).reshape([-1 if axis == dim else 1 for axis in range(len(shape))])
    return loudness


def bell_draw(rng, extent, scale, limit, cuts=(), kind=jnp.bfloat16):
    factor_of = level_of(rng, extent, cuts, -0.22, 0.18) if cuts else 1.0
    drawn = jax.random.normal(rng, extent, jnp.float32) * scale * factor_of
    return jnp.minimum(jnp.maximum(drawn, -limit), limit).astype(kind)


def setup_inputs(seed: int = 0) -> dict:
    keys = jax.random.split(jax.random.key(seed), 21)
    return {
        "latents": draw_latents(jax.random.fold_in(keys[20], 71), 0),
        "context": draw_context(jax.random.fold_in(keys[20], 71), 0),
        "cond_vec": bell_draw(keys[2], (MODEL_WIDTH,), 1.0, 6.0, (), jnp.float32),
        "ctx_vec": bell_draw(keys[3], (MODEL_WIDTH,), 1.0, 6.0, (), jnp.float32),
        "shift_w": bell_draw(keys[4], (MODEL_WIDTH, MODEL_WIDTH), MODEL_WIDTH ** -0.5, 0.125, ((0, 8), (1, 4))),
        "scale_w": bell_draw(keys[5], (MODEL_WIDTH, MODEL_WIDTH), MODEL_WIDTH ** -0.5, 0.125, ((0, 8), (1, 4))),
        "modgate_w": bell_draw(keys[6], (MODEL_WIDTH, MODEL_WIDTH), MODEL_WIDTH ** -0.5, 0.125, ((0, 8), (1, 4))),
        "query_down_weight": bell_draw(keys[7], (MODEL_WIDTH, QUERY_LATENT), MODEL_WIDTH ** -0.5, 0.125),
        "latent_down_weight": bell_draw(keys[8], (MODEL_WIDTH, LATENT_WIDTH), MODEL_WIDTH ** -0.5, 0.125),
        "rot_down": bell_draw(keys[9], (MODEL_WIDTH, ROTARY_SIZE), MODEL_WIDTH ** -0.5, 0.125),
        "gate_w": bell_draw(keys[10], (MODEL_WIDTH, HEAD_COUNT * VALUE_HEAD_SIZE), MODEL_WIDTH ** -0.5, 0.125, ((1, 4),)),
        "query_norm_gain": jnp.clip(1.0 + 0.18 * jax.random.normal(keys[11], (QUERY_LATENT,), jnp.float32), 0.1, 1.9),
        "latent_norm_gain": jnp.clip(1.0 + 0.18 * jax.random.normal(keys[12], (LATENT_WIDTH,), jnp.float32), 0.1, 1.9),
        "query_plain_weight": bell_draw(keys[13], (QUERY_LATENT, HEAD_COUNT * PLAIN_HEAD_SIZE), QUERY_LATENT ** -0.5, 0.25, ((1, 4),)),
        "query_rotary_weight": bell_draw(keys[14], (QUERY_LATENT, HEAD_COUNT * ROTARY_SIZE), QUERY_LATENT ** -0.5, 0.25, ((1, 4),)),
        "key_expand_weight": bell_draw(keys[15], (LATENT_WIDTH, HEAD_COUNT * PLAIN_HEAD_SIZE), LATENT_WIDTH ** -0.5, 0.375, ((1, 4),)),
        "value_expand_weight": bell_draw(keys[16], (LATENT_WIDTH, HEAD_COUNT * VALUE_HEAD_SIZE), LATENT_WIDTH ** -0.5, 0.375, ((1, 4),)),
        "out_w": bell_draw(keys[17], (HEAD_COUNT * VALUE_HEAD_SIZE, MODEL_WIDTH), (HEAD_COUNT * VALUE_HEAD_SIZE // 16) ** -0.5, 0.5, ((0, 4),)),
        "norm_gain": jnp.clip(1.0 + 0.18 * jax.random.normal(keys[18], (MODEL_WIDTH,), jnp.float32), 0.1, 1.9),
        "norm_bias": bell_draw(keys[19], (MODEL_WIDTH,), 0.5, 3.0, (), jnp.float32),
    }


rope_base = 10000.0
norm_floor = 1e-06
residual_weight = 2.0 ** 0.5

def rms_scale(values, gain):
    return values * lax.rsqrt(lax.optimization_barrier(jnp.mean(values * values, axis=-1, keepdims=True)) + norm_floor) * gain

def rotate(values, positions):
    pair_count = ROTARY_SIZE // 4
    inverse = rope_base ** (-jnp.arange(pair_count, dtype=jnp.float32) / pair_count)
    grid_row = (positions // GRID_W).astype(jnp.float32)
    grid_col = (positions % GRID_W).astype(jnp.float32)
    angles = jnp.stack([grid_row[:, None] * inverse, grid_col[:, None] * inverse], axis=1)
    cosine = jnp.cos(angles)[:, None, :, None, :]
    sine_part = jnp.sin(angles)[:, None, :, None, :]
    shaped = values.reshape(values.shape[0], -1, 2, 2, pair_count)
    first_part = shaped[:, :, :, 0:1, :]
    second = shaped[:, :, :, 1:2, :]
    turned = jnp.concatenate([first_part * cosine - second * sine_part, second * cosine + first_part * sine_part], axis=3)
    return turned.reshape(values.shape)

def project(rows, weight):
    return jnp.dot(rows, weight, preferred_element_type=jnp.float32)

def reference(latents, context, cond_vec, ctx_vec, shift_w, scale_w, modgate_w, query_down_weight, latent_down_weight, rot_down, gate_w, query_norm_gain, latent_norm_gain, query_plain_weight, query_rotary_weight, key_expand_weight, value_expand_weight, out_w, norm_gain, norm_bias):
    cond_rows = jnp.stack([jax.nn.silu(cond_vec), jax.nn.silu(ctx_vec)]).astype(jnp.bfloat16)
    shift_vec = project(cond_rows, shift_w)
    scale_vec = project(cond_rows, scale_w)
    gate_vec = project(cond_rows, modgate_w)
    latent_in = (latents.astype(jnp.float32) * (1.0 + scale_vec[0]) + shift_vec[0]).astype(jnp.bfloat16)
    context_in = (context.astype(jnp.float32) * (1.0 + scale_vec[1]) + shift_vec[1]).astype(jnp.bfloat16)
    positions = jnp.arange(TOKENS, dtype=jnp.int32)
    q_codes = rms_scale(project(latent_in, query_down_weight), query_norm_gain).astype(jnp.bfloat16)
    q_cont = project(q_codes, query_plain_weight).astype(jnp.bfloat16).reshape(TOKENS, HEAD_COUNT, PLAIN_HEAD_SIZE)
    q_rot = rotate(project(q_codes, query_rotary_weight), positions).astype(jnp.bfloat16).reshape(TOKENS, HEAD_COUNT, ROTARY_SIZE)
    gate_act = project(latent_in, gate_w).astype(jnp.bfloat16)
    all_in = jnp.concatenate([context_in, latent_in], axis=0)
    kv_codes = rms_scale(project(all_in, latent_down_weight), latent_norm_gain).astype(jnp.bfloat16)
    key_rot = jnp.concatenate([project(context_in, rot_down), rotate(project(latent_in, rot_down), positions)], axis=0).astype(jnp.bfloat16)
    key_rows = project(kv_codes, key_expand_weight).astype(jnp.bfloat16).reshape(-1, HEAD_COUNT, PLAIN_HEAD_SIZE).astype(jnp.float32)
    value_rows = project(kv_codes, value_expand_weight).astype(jnp.bfloat16).reshape(-1, HEAD_COUNT, VALUE_HEAD_SIZE).astype(jnp.float32)
    rot_wide = key_rot.astype(jnp.float32)
    score_scale = (PLAIN_HEAD_SIZE + ROTARY_SIZE) ** (-0.5)
    block_rows = TOK_DEV // N_TP

    def attend_block(inputs):
        cont_block, rot_block = inputs
        scores = jnp.einsum('qhd,khd->hqk', cont_block.astype(jnp.float32), key_rows)
        scores = (scores + jnp.einsum('qhd,kd->hqk', rot_block.astype(jnp.float32), rot_wide)) * score_scale
        weights = jnp.exp(scores - lax.optimization_barrier(jnp.max(scores, axis=-1, keepdims=True)))
        weights_low = lax.optimization_barrier(weights.astype(jnp.bfloat16)).astype(jnp.float32)
        weighted = jnp.einsum('hqk,khd->qhd', weights_low, value_rows)
        return weighted / jnp.transpose(lax.optimization_barrier(jnp.sum(weights, axis=-1)))[:, :, None]
    blocks = TOKENS // block_rows
    attended = lax.map(attend_block, (q_cont.reshape(blocks, block_rows, HEAD_COUNT, PLAIN_HEAD_SIZE), q_rot.reshape(blocks, block_rows, HEAD_COUNT, ROTARY_SIZE)))
    attended = attended.reshape(TOKENS, HEAD_COUNT * VALUE_HEAD_SIZE)
    gated = (attended * jax.nn.silu(gate_act.astype(jnp.float32))).astype(jnp.bfloat16)
    branch = project(gated, out_w)
    blended = residual_weight * latents.astype(jnp.float32) + gate_vec[0] * branch
    row_mean = lax.optimization_barrier(jnp.mean(blended, axis=-1, keepdims=True))
    centred = blended - row_mean
    row_var = lax.optimization_barrier(jnp.mean(centred * centred, axis=-1, keepdims=True))
    return (centred * lax.rsqrt(row_var + norm_floor) * norm_gain + norm_bias).astype(jnp.bfloat16)
```

```python
import math

import jax
import jax.numpy as jnp
from jax import lax
from jax.experimental import pallas as pl
from jax.experimental.pallas import tpu as pltpu
from jax.sharding import PartitionSpec as P

HEAD = 64
ROT = 32
GRID_W = 64
LANES = 128

rope_base = 10000.0
norm_floor = 1e-06
residual_weight = 2.0**0.5
F32 = jnp.float32
BF16 = jnp.bfloat16
MESH = pl.DeviceIdType.MESH


def dot(a, b):
    return jnp.dot(a, b, preferred_element_type=F32)


def ring_pos(sp, n):
    return jnp.where(sp % 2 == 0, sp // 2, n - 1 - sp // 2)


def ring_sp(r, n):
    return jnp.where(r < n // 2, 2 * r, 2 * (n - 1 - r) + 1)


def lane_iota(shape):
    return lax.broadcasted_iota(jnp.int32, shape, len(shape) - 1)


def make_kernel(n_sp, n_tp, rows, ctx_rows, width, heads):
    seq = rows * n_tp
    block = seq + ctx_rows
    half = block // 2
    n_x = n_tp // 2
    pairs = heads // 2
    q_groups = (heads * ROT) // LANES
    mod_cols = width // n_tp
    score_scale = (HEAD + ROT) ** (-0.5) * math.log2(math.e)
    last = n_sp // 2

    def kernel(
        lat_hbm, ctx_hbm, cond, shift_hbm, scale_hbm, mgate_hbm, qd_hbm, ld_hbm, rd_hbm, gw_hbm,
        q_gain, l_gain, qp_hbm, qr_hbm, ke_hbm, ve_hbm, ow_hbm, n_gain, n_bias,
        out,
        lat, ctx, w_shift, w_scale, w_mgate, qd, ld, rd, gw, qp, qr, ke, ve, ow,
        modbuf, vecs, X, cosb, sinb, codes, Q, gate, M, O, gated, pair_out, pair_in, x_out, x_in,
        own_acc,
        ld_sem, mod_s, mod_r, vec_s, vec_r, lat_s, lat_r, rel_s, rel_r,
        rr_s, rr_r, rl_s, rl_r, dr_s, dr_r, dl_s, dl_r, pr_s, pr_r, xs_s, xs_r,
    ):
        sp = lax.axis_index("sp")
        tp = lax.axis_index("tp")
        core = tp % 2
        xi = tp // 2
        partner = xi * 2 + (1 - core)
        r = ring_pos(sp, n_sp)

        loads = []

        def load(src, dst):
            c = pltpu.make_async_copy(src, dst, ld_sem.at[len(loads)])
            c.start()
            loads.append(c)
            return c

        l_mod = [load(shift_hbm, w_shift), load(scale_hbm, w_scale), load(mgate_hbm, w_mgate)]
        l_lat = load(lat_hbm, lat.at[tp])
        l_ctx = load(ctx_hbm, ctx)
        l_ld = load(ld_hbm, ld)
        l_rd = load(rd_hbm, rd)
        l_qd = load(qd_hbm, qd)
        l_gw = load(gw_hbm, gw)
        l_q = [load(qp_hbm, qp), load(qr_hbm, qr)]
        l_kv = [load(ke_hbm, ke), load(ve_hbm, ve)]
        l_ow = load(ow_hbm, ow)

        bar = pltpu.get_barrier_semaphore()
        for d in range(1, n_sp):
            pl.semaphore_signal(bar, inc=1, device_id=((sp + d) % n_sp, tp), device_id_type=MESH)
        for d in range(1, n_tp):
            pl.semaphore_signal(bar, inc=1, device_id=(sp, (tp + d) % n_tp), device_id_type=MESH)

        for c in l_mod:
            c.wait()
        modbuf[sp] = jnp.zeros((8, mod_cols), F32)
        cv = cond[...]
        for i, w in enumerate((w_shift, w_scale, w_mgate)):
            modbuf[sp, 2 * i : 2 * i + 2, :] = dot(cv, w[...])[0:2]
        pl.semaphore_wait(bar, n_sp + n_tp - 2)

        def remote(src, dst, s, rcv, dev):
            return pltpu.make_async_remote_copy(
                src_ref=src, dst_ref=dst, send_sem=s, recv_sem=rcv, device_id=dev, device_id_type=MESH
            )

        sends = []
        for d in range(1, n_sp):
            k = (sp + d) % n_sp
            c = remote(modbuf.at[sp], modbuf.at[sp], mod_s.at[d], mod_r.at[sp], (k, tp))
            c.start()
            sends.append(c)
        l_lat.wait()
        for d in range(1, n_x):
            k = ((xi + d) % n_x) * 2 + core
            c = remote(lat.at[tp], lat.at[tp], lat_s.at[d], lat_r.at[tp], (sp, k))
            c.start()
            sends.append(c)
        c = remote(lat.at[tp], lat.at[tp], lat_s.at[0], lat_r.at[tp], (sp, partner))
        c.start()
        sends.append(c)

        lane = lane_iota((seq, LANES))
        pos = sp * seq + lax.broadcasted_iota(jnp.int32, (seq, LANES), 0)
        pair_no = (lane % 8).astype(F32)
        inv = jnp.exp(pair_no * (-math.log(rope_base) / 8))
        grid_row = pos // GRID_W
        grid_col = pos - grid_row * GRID_W
        where_axis = jnp.where((lane % 32) < 16, grid_row, grid_col).astype(F32)
        ang = where_axis * inv
        cosb[...] = jnp.cos(ang)
        sinb[...] = jnp.where((lane % 16) < 8, -jnp.sin(ang), jnp.sin(ang))

        def rotate(v):
            ln = lane_iota(v.shape)
            sw = jnp.where((ln % 16) < 8, pltpu.roll(v, LANES - 8, 1), pltpu.roll(v, 8, 1))
            return v * cosb[...] + sw * sinb[...]

        for d in range(1, n_sp):
            k = (sp + d) % n_sp
            remote(modbuf.at[k], modbuf.at[k], mod_s.at[d], mod_r.at[k], (k, tp)).wait_recv()
        tot = modbuf[0]
        for k in range(1, n_sp):
            tot = tot + modbuf[k]
        vecs[tp] = tot
        for d in range(1, n_tp):
            k = (tp + d) % n_tp
            c = remote(vecs.at[tp], vecs.at[tp], vec_s.at[d], vec_r.at[tp], (sp, k))
            c.start()
            sends.append(c)
        for d in range(1, n_x):
            k = ((xi + d) % n_x) * 2 + core
            remote(lat.at[k], lat.at[k], lat_s.at[d], lat_r.at[k], (sp, k)).wait_recv()
            c = remote(lat.at[k], lat.at[k], rel_s.at[d], rel_r.at[k], (sp, partner))
            c.start()
            sends.append(c)
        for d in range(1, n_tp):
            k = (tp + d) % n_tp
            remote(vecs.at[k], vecs.at[k], vec_s.at[d], vec_r.at[k], (sp, k)).wait_recv()

        def vec_row(i):
            return jnp.concatenate([vecs[t, i : i + 1, :] for t in range(n_tp)], axis=1)

        shift0, shift1 = vec_row(0), vec_row(1)
        scale0, scale1 = 1.0 + vec_row(2), 1.0 + vec_row(3)
        l_ctx.wait()
        X[seq:block, :] = (ctx[...].astype(F32) * scale1 + shift1).astype(BF16)
        remote(lat.at[partner], lat.at[partner], lat_s.at[0], lat_r.at[partner], (sp, partner)).wait_recv()
        for d in range(1, n_x):
            k = ((xi + d) % n_x) * 2 + (1 - core)
            remote(lat.at[k], lat.at[k], rel_s.at[d], rel_r.at[k], (sp, partner)).wait_recv()
        for t in range(n_tp):
            X[t * rows : (t + 1) * rows, :] = (lat[t].astype(F32) * scale0 + shift0).astype(BF16)

        def rms(v, g):
            return v * lax.rsqrt(jnp.mean(v * v, axis=-1, keepdims=True) + norm_floor) * g

        l_ld.wait()
        l_rd.wait()
        lat_w = ld.shape[1]
        codes[r, :, 0:lat_w] = rms(dot(X[...], ld[...]), l_gain[...]).astype(BF16)
        kr = dot(X[...], rd[...])
        kr4 = jnp.concatenate([kr, kr, kr, kr], axis=1)
        codes[r, 0:seq, lat_w : lat_w + LANES] = rotate(kr4[0:seq]).astype(BF16)
        codes[r, seq:block, lat_w : lat_w + LANES] = kr4[seq:block].astype(BF16)

        right = ring_sp((r + 1) % n_sp, n_sp)
        left = ring_sp((r + n_sp - 1) % n_sp, n_sp)

        def part(owner, c):
            return codes.at[owner, pl.ds(pl.multiple_of(c * half, 16), half), :]

        def right_copy(owner, s):
            return remote(part(owner, core), part(owner, core), rr_s.at[s], rr_r.at[s], (right, tp))

        def left_copy(owner, s):
            return remote(part(owner, core), part(owner, core), rl_s.at[s], rl_r.at[s], (left, tp))

        def hand_right(owner, s, c):
            return remote(part(owner, c), part(owner, c), dr_s.at[s], dr_r.at[s], (sp, partner))

        def hand_left(owner, s, c):
            return remote(part(owner, c), part(owner, c), dl_s.at[s], dl_r.at[s], (sp, partner))

        right_copy(r, 1).start()
        left_copy(r, 1).start()

        l_qd.wait()
        qc = rms(dot(X[0:seq, :], qd[...]), q_gain[...]).astype(BF16)
        for c in l_q:
            c.wait()
        q_plain = dot(qc, qp[...]).astype(BF16)
        q_rotary = dot(qc, qr[...])
        lane_q = lane_iota((seq, LANES))
        for g in range(q_groups):
            turned = rotate(q_rotary[:, g * LANES : (g + 1) * LANES]).astype(BF16)
            for i in range(LANES // ROT):
                h = g * (LANES // ROT) + i
                lo = (h // 2) * LANES
                plain = q_plain[:, lo : lo + LANES]
                Q[h, :, 0:LANES] = jnp.where((lane_q // HEAD) == h % 2, plain, jnp.zeros_like(plain))
                Q[h, :, LANES : 2 * LANES] = jnp.where(
                    (lane_q // ROT) == i, turned, jnp.zeros_like(turned)
                )
        l_gw.wait()
        gate[...] = dot(X[0:seq, :], gw[...]).astype(BF16)

        for h in range(heads):
            M[h] = jnp.full((seq, LANES), -1e30, F32)
            O[h] = jnp.zeros((seq, LANES), F32)
        for c in l_kv:
            c.wait()

        def attend(owner):
            cd = codes[owner, :, 0:lat_w]
            rt = codes[owner, :, lat_w : lat_w + LANES]

            def one_pair(p, carry):
                cols = pl.ds(pl.multiple_of(p * LANES, LANES), LANES)
                kp = dot(cd, ke[:, cols]).astype(BF16)
                vp = dot(cd, ve[:, cols]).astype(BF16)
                kc = jnp.concatenate([kp, rt], axis=1)
                ln = lane_iota(vp.shape)
                for e in range(2):
                    h = 2 * p + e
                    s = lax.dot_general(
                        Q[h], kc, (((1,), (1,)), ((), ())), preferred_element_type=F32
                    )
                    top = M[h]
                    new = jnp.maximum(top, jnp.max(s, axis=1, keepdims=True))
                    M[h] = new
                    alpha = jnp.exp2((top - new) * score_scale)
                    w = jnp.exp2((s - new[:, 0:1]) * score_scale).astype(BF16)
                    v = jnp.where((ln // HEAD) == e, vp, jnp.ones_like(vp))
                    O[h] = O[h] * alpha + dot(w, v)
                return carry

            lax.fori_loop(0, pairs, one_pair, 0)

        attend(r)

        def step(s, carry):
            from_left = (r + n_sp - s) % n_sp
            from_right = (r + s) % n_sp
            right_copy(from_left, s).wait_recv()
            right_copy(from_left, s + 1).start()
            hand_right(from_left, s, core).start()
            left_copy(from_right, s).wait_recv()

            @pl.when(s < last - 1)
            def _():
                left_copy(from_right, s + 1).start()

            hand_left(from_right, s, core).start()
            hand_right(from_left, s, 1 - core).wait_recv()
            attend(from_left)
            hand_left(from_right, s, 1 - core).wait_recv()
            attend(from_right)
            return carry

        lax.fori_loop(1, last, step, 0)
        far = (r + n_sp - last) % n_sp
        right_copy(far, last).wait_recv()
        hand_right(far, last, core).start()
        hand_right(far, last, 1 - core).wait_recv()
        attend(far)

        ln2 = lane_iota((seq, LANES))
        for p in range(pairs):
            a, b = O[2 * p], O[2 * p + 1]
            num = jnp.where(ln2 < HEAD, a, b)
            den = pltpu.roll(jnp.where(ln2 < HEAD, b, a), HEAD, 1)
            gt = gate[:, p * LANES : (p + 1) * LANES].astype(F32)
            act = gt / (1.0 + jnp.exp(-gt))
            gated[:, p * LANES : (p + 1) * LANES] = (num / den * act).astype(BF16)

        l_ow.wait()

        def branch(t):
            return dot(gated[pl.ds(pl.multiple_of(t * rows, 16), rows), :], ow[...])

        for d in range(1, n_x + 1):
            x2 = (xi + d) % n_x
            pair_out[d - 1] = branch(x2 * 2 + 1 - core).astype(BF16)
            c = remote(pair_out.at[d - 1], pair_in.at[d - 1], pr_s.at[d - 1], pr_r.at[d - 1], (sp, partner))
            c.start()
            sends.append(c)
        for d in range(1, n_x + 1):
            x2 = (xi + d) % n_x
            mine = branch(x2 * 2 + core)
            remote(
                pair_out.at[d - 1], pair_in.at[d - 1], pr_s.at[d - 1], pr_r.at[d - 1], (sp, partner)
            ).wait_recv()
            mine = mine + pair_in[d - 1].astype(F32)
            if d < n_x:
                x_out[d - 1] = mine.astype(BF16)
                c = remote(x_out.at[d - 1], x_in.at[d - 1], xs_s.at[d - 1], xs_r.at[d - 1], (sp, x2 * 2 + core))
                c.start()
                sends.append(c)
            else:
                own_acc[...] = mine
        acc = own_acc[...]
        for d in range(1, n_x):
            x2 = (xi + d) % n_x
            remote(
                x_out.at[d - 1], x_in.at[d - 1], xs_s.at[d - 1], xs_r.at[d - 1], (sp, x2 * 2 + core)
            ).wait_recv()
            acc = acc + x_in[d - 1].astype(F32)
        blended = residual_weight * lat[tp].astype(F32) + vec_row(4) * acc
        centred = blended - jnp.mean(blended, axis=-1, keepdims=True)
        var = jnp.mean(centred * centred, axis=-1, keepdims=True)
        out[...] = (centred * lax.rsqrt(var + norm_floor) * n_gain[...] + n_bias[...]).astype(BF16)

        for c in sends:
            c.wait_send()
        right_copy(r, 1).wait_send()
        left_copy(r, 1).wait_send()

        def drain(s, carry):
            right_copy(r, s + 1).wait_send()
            hand_right(r, s, core).wait_send()
            hand_left(r, s, core).wait_send()

            @pl.when(s < last - 1)
            def _():
                left_copy(r, s + 1).wait_send()

            return carry

        lax.fori_loop(1, last, drain, 0)
        hand_right(r, last, core).wait_send()

    def scratch():
        bf = lambda *s: pltpu.VMEM(s, BF16)
        f3 = lambda *s: pltpu.VMEM(s, F32)
        sem = lambda k: pltpu.SemaphoreType.DMA((k,))
        slab = width // n_sp
        return bf, f3, sem, slab

    return kernel, scratch, seq, block


def per_device(
    latents, context, cond_vec, ctx_vec, shift_w, scale_w, modgate_w, query_down_weight,
    latent_down_weight, rot_down, gate_w, query_norm_gain, latent_norm_gain, query_plain_weight,
    query_rotary_weight, key_expand_weight, value_expand_weight, out_w, norm_gain, norm_bias,
):
    n_sp, n_tp = lax.axis_size("sp"), lax.axis_size("tp")
    rows, width = latents.shape
    ctx_rows = context.shape[0]
    hcols = gate_w.shape[1]
    heads = hcols // HEAD
    slab = shift_w.shape[0]
    kernel, scratch, seq, block = make_kernel(n_sp, n_tp, rows, ctx_rows, width, heads)
    bf, f3, sem, _ = scratch()
    cond_rows = jnp.stack([jax.nn.silu(cond_vec), jax.nn.silu(ctx_vec)]).astype(BF16)
    cond_here = lax.dynamic_slice_in_dim(cond_rows, lax.axis_index("sp") * slab, slab, 1)
    cond_here = jnp.pad(cond_here, ((0, 14), (0, 0)))
    n_x = n_tp // 2
    last = n_sp // 2
    lat_w = latent_down_weight.shape[1]
    any_spec = pl.BlockSpec(memory_space=pl.ANY)
    vm = pl.BlockSpec(memory_space=pltpu.VMEM)
    call = pl.pallas_call(
        kernel,
        out_shape=jax.ShapeDtypeStruct((rows, width), BF16),
        in_specs=[any_spec] * 2 + [vm] + [any_spec] * 7 + [vm] * 2 + [any_spec] * 5 + [vm] * 2,
        out_specs=vm,
        scratch_shapes=[
            bf(n_tp, rows, width), bf(*context.shape), bf(*shift_w.shape), bf(*scale_w.shape),
            bf(*modgate_w.shape), bf(*query_down_weight.shape), bf(*latent_down_weight.shape),
            bf(*rot_down.shape), bf(*gate_w.shape), bf(*query_plain_weight.shape),
            bf(*query_rotary_weight.shape), bf(*key_expand_weight.shape),
            bf(*value_expand_weight.shape), bf(*out_w.shape),
            f3(n_sp, 8, width // n_tp), f3(n_tp, 8, width // n_tp), bf(block, width),
            f3(seq, LANES), f3(seq, LANES), bf(n_sp, block, lat_w + LANES),
            bf(heads, seq, 2 * LANES), bf(seq, hcols), f3(heads, seq, LANES), f3(heads, seq, LANES),
            bf(seq, hcols), bf(n_x, rows, width), bf(n_x, rows, width), bf(n_x, rows, width),
            bf(n_x, rows, width), f3(rows, width),
            sem(16), sem(n_sp), sem(n_sp), sem(n_tp), sem(n_tp), sem(n_x), sem(n_tp), sem(n_x), sem(n_tp),
            sem(last + 1), sem(last + 1), sem(last + 1), sem(last + 1),
            sem(last + 1), sem(last + 1), sem(last + 1), sem(last + 1),
            sem(n_x), sem(n_x), sem(n_x), sem(n_x),
        ],
        compiler_params=pltpu.CompilerParams(
            collective_id=0, has_side_effects=True, vmem_limit_bytes=62 * 1024 * 1024
        ),
    )
    return call(
        latents, context, cond_here, shift_w, scale_w, modgate_w, query_down_weight,
        latent_down_weight, rot_down, gate_w, query_norm_gain.reshape(1, -1),
        latent_norm_gain.reshape(1, -1), query_plain_weight, query_rotary_weight,
        key_expand_weight, value_expand_weight, out_w, norm_gain.reshape(1, -1),
        norm_bias.reshape(1, -1),
    )


def solution(mesh):
    in_specs = (
        P(("sp", "tp"), None), P("sp", None), P(), P(), P("sp", "tp"), P("sp", "tp"), P("sp", "tp"),
        P(), P(), P(), P(None, "tp"), P(), P(), P(None, "tp"), P(None, "tp"), P(None, "tp"),
        P(None, "tp"), P("tp", None), P(), P(),
    )
    return jax.shard_map(
        per_device, mesh=mesh, in_specs=in_specs, out_specs=P(("sp", "tp"), None), check_vma=False
    )
```

```python
import math

import jax
import jax.numpy as jnp
from jax import lax
from jax.experimental import pallas as pl
from jax.experimental.pallas import tpu as pltpu
from jax.sharding import PartitionSpec as P

HEAD = 64
ROT = 32
GRID_W = 64
LANES = 128

rope_base = 10000.0
norm_floor = 1e-06
residual_weight = 2.0**0.5
F32 = jnp.float32
BF16 = jnp.bfloat16
MESH = pl.DeviceIdType.MESH


def dot(a, b):
    return jnp.dot(a, b, preferred_element_type=F32)


def ring_pos(sp, n):
    return jnp.where(sp % 2 == 0, sp // 2, n - 1 - sp // 2)


def ring_sp(r, n):
    return jnp.where(r < n // 2, 2 * r, 2 * (n - 1 - r) + 1)


def lane_iota(shape):
    return lax.broadcasted_iota(jnp.int32, shape, len(shape) - 1)


def make_kernel(n_sp, n_tp, rows, ctx_rows, width, heads):
    seq = rows * n_tp
    block = seq + ctx_rows
    half = block // 2
    n_x = n_tp // 2
    pairs = heads // 2
    q_groups = (heads * ROT) // LANES
    mod_cols = width // n_tp
    score_scale = (HEAD + ROT) ** (-0.5) * math.log2(math.e)
    last = n_sp // 2

    def kernel(
        lat_hbm, ctx_hbm, cond0, cond1, shift_hbm, scale_hbm, mgate_hbm, qd_hbm, ld_hbm, rd_hbm, gw_hbm,
        q_gain, l_gain, qp_hbm, qr_hbm, ke_hbm, ve_hbm, ow_hbm, n_gain, n_bias,
        out,
        lat, ctx, w_shift, w_scale, w_mgate, qd, ld, rd, gw, qp, qr, kv, ow,
        modbuf, vecs, X, cosb, sinb, codes, Q, gate, M, O, gated, pair_out, pair_in, x_out, x_in,
        own_acc,
        ld_sem, mod_s, mod_r, vec_s, vec_r, lat_s, lat_r, rel_s, rel_r, own_s, own_r,
        rr_s, rr_r, rl_s, rl_r, dr_s, dr_r, dl_s, dl_r, pr_s, pr_r, xs_s, xs_r,
    ):
        sp = lax.axis_index("sp")
        tp = lax.axis_index("tp")
        core = tp % 2
        xi = tp // 2
        partner = xi * 2 + (1 - core)
        r = ring_pos(sp, n_sp)

        loads = []

        def load(src, dst):
            c = pltpu.make_async_copy(src, dst, ld_sem.at[len(loads)])
            c.start()
            loads.append(c)
            return c

        l_mod = [load(shift_hbm, w_shift), load(scale_hbm, w_scale), load(mgate_hbm, w_mgate)]
        l_lat = load(lat_hbm, lat.at[tp])
        l_ctx = load(ctx_hbm, ctx)
        l_ld = load(ld_hbm, ld)
        l_rd = load(rd_hbm, rd)
        l_qd = load(qd_hbm, qd)
        l_gw = load(gw_hbm, gw)
        l_q = [load(qp_hbm, qp), load(qr_hbm, qr)]
        l_kv = []
        for p in range(pairs):
            cols = pl.ds(p * LANES, LANES)
            l_kv.append(load(ke_hbm.at[:, cols], kv.at[p, :, pl.ds(0, LANES)]))
            l_kv.append(load(ve_hbm.at[:, cols], kv.at[p, :, pl.ds(LANES, LANES)]))
        l_ow = load(ow_hbm, ow)

        bar = pltpu.get_barrier_semaphore()
        for d in range(1, n_sp):
            pl.semaphore_signal(bar, inc=1, device_id=((sp + d) % n_sp, tp), device_id_type=MESH)
        for d in range(1, n_tp):
            pl.semaphore_signal(bar, inc=1, device_id=(sp, (tp + d) % n_tp), device_id_type=MESH)

        for c in l_mod:
            c.wait()
        modbuf[sp] = jnp.zeros((8, mod_cols), F32)
        slab = w_shift.shape[0]

        def slab_of(ref):
            if slab % LANES == 0:
                return ref[:, pl.ds(pl.multiple_of(sp * slab, LANES), slab)]
            per = LANES // slab
            window = ref[:, pl.ds(pl.multiple_of(sp // per * LANES, LANES), LANES)]
            v = window[:, 0:slab]
            for i in range(1, per):
                v = jnp.where(sp % per == i, window[:, i * slab : (i + 1) * slab], v)
            return v

        def silu(v):
            return v / (1.0 + jnp.exp(-v))

        row_no = lax.broadcasted_iota(jnp.int32, (16, slab), 0)
        cv = jnp.where(row_no == 0, silu(slab_of(cond0)), silu(slab_of(cond1))).astype(BF16)
        for i, w in enumerate((w_shift, w_scale, w_mgate)):
            modbuf[sp, 2 * i : 2 * i + 2, :] = dot(cv, w[...])[0:2]
        pl.semaphore_wait(bar, n_sp + n_tp - 2)

        def remote(src, dst, s, rcv, dev):
            return pltpu.make_async_remote_copy(
                src_ref=src, dst_ref=dst, send_sem=s, recv_sem=rcv, device_id=dev, device_id_type=MESH
            )

        sends = []
        for d in range(1, n_sp):
            k = (sp + d) % n_sp
            c = remote(modbuf.at[sp], modbuf.at[sp], mod_s.at[d], mod_r.at[sp], (k, tp))
            c.start()
            sends.append(c)
        l_lat.wait()
        early = rows // 2 // 16 * 16
        pieces = (pl.ds(0, early), pl.ds(early, rows - early))

        def lat_copy(owner, i, d, k):
            return remote(
                lat.at[owner, pieces[i]], lat.at[owner, pieces[i]], lat_s.at[2 * d + i],
                lat_r.at[2 * owner + i], (sp, k),
            )

        def relay_copy(owner, i, d):
            return remote(
                lat.at[owner, pieces[i]], lat.at[owner, pieces[i]], rel_s.at[2 * d + i],
                rel_r.at[2 * owner + i], (sp, partner),
            )

        def own_copy(owner):
            return remote(lat.at[owner], lat.at[owner], own_s.at[0], own_r.at[0], (sp, partner))

        def send_piece(i):
            for d in range(1, n_x):
                c = lat_copy(tp, i, d, ((xi + d) % n_x) * 2 + core)
                c.start()
                sends.append(c)

        send_piece(0)
        c = own_copy(tp)
        c.start()
        sends.append(c)

        lane = lane_iota((seq, LANES))
        pos = sp * seq + lax.broadcasted_iota(jnp.int32, (seq, LANES), 0)
        pair_no = (lane % 8).astype(F32)
        inv = jnp.exp(pair_no * (-math.log(rope_base) / 8))
        grid_row = pos // GRID_W
        grid_col = pos - grid_row * GRID_W
        where_axis = jnp.where((lane % 32) < 16, grid_row, grid_col).astype(F32)
        ang = where_axis * inv
        cosb[...] = jnp.cos(ang)
        sinb[...] = jnp.where((lane % 16) < 8, -jnp.sin(ang), jnp.sin(ang))

        def rotate(v, at):
            ln = lane_iota(v.shape)
            sw = jnp.where((ln % 16) < 8, pltpu.roll(v, LANES - 8, 1), pltpu.roll(v, 8, 1))
            return v * cosb[at, :] + sw * sinb[at, :]

        for d in range(1, n_sp):
            k = (sp + d) % n_sp
            remote(modbuf.at[k], modbuf.at[k], mod_s.at[d], mod_r.at[k], (k, tp)).wait_recv()
        tot = modbuf[0]
        for k in range(1, n_sp):
            tot = tot + modbuf[k]
        vecs[tp] = tot
        for d in range(1, n_tp):
            k = (tp + d) % n_tp
            c = remote(vecs.at[tp], vecs.at[tp], vec_s.at[d], vec_r.at[tp], (sp, k))
            c.start()
            sends.append(c)
        send_piece(1)
        for d in range(1, n_tp):
            k = (tp + d) % n_tp
            remote(vecs.at[k], vecs.at[k], vec_s.at[d], vec_r.at[k], (sp, k)).wait_recv()

        def vec_row(i):
            return jnp.concatenate([vecs[t, i : i + 1, :] for t in range(n_tp)], axis=1)

        shift0, shift1 = vec_row(0), vec_row(1)
        scale0, scale1 = 1.0 + vec_row(2), 1.0 + vec_row(3)
        chip_rows = 2 * rows
        lat_w = ld.shape[1]

        def rms(v, g):
            return v * lax.rsqrt(jnp.mean(v * v, axis=-1, keepdims=True) + norm_floor) * g

        def chip_at(x):
            return pl.ds(pl.multiple_of(x * chip_rows, 16), chip_rows)

        def encode(at, turn):
            v = X[at, :]
            codes[r, at, 0:lat_w] = rms(dot(v, ld[...]), l_gain[...]).astype(BF16)
            kr = lax.dot_general(v, rd[...], (((1,), (1,)), ((), ())), preferred_element_type=F32)
            kr = jnp.concatenate([kr] * (LANES // ROT), axis=1)
            codes[r, at, lat_w : lat_w + LANES] = (rotate(kr, at) if turn else kr).astype(BF16)

        def modulate(x):
            for c in range(2):
                t = 2 * x + c
                X[pl.ds(pl.multiple_of(t * rows, 8), rows), :] = (
                    lat[t].astype(F32) * scale0 + shift0
                ).astype(BF16)

        def queries(x):
            at = chip_at(x)
            v = X[at, :]
            qc = rms(dot(v, qd[...]), q_gain[...]).astype(BF16)
            q_plain = (dot(qc, qp[...]) * score_scale).astype(BF16)
            q_rotary = dot(qc, qr[...]) * score_scale
            lane_q = lane_iota((chip_rows, LANES))
            for g in range(q_groups):
                turned = rotate(q_rotary[:, g * LANES : (g + 1) * LANES], at).astype(BF16)
                for i in range(LANES // ROT):
                    h = g * (LANES // ROT) + i
                    lo = (h // 2) * LANES
                    plain = q_plain[:, lo : lo + LANES]
                    Q[h, at, 0:LANES] = jnp.where((lane_q // HEAD) == h % 2, plain, jnp.zeros_like(plain))
                    Q[h, at, LANES : 2 * LANES] = jnp.where(
                        (lane_q // ROT) == i, turned, jnp.zeros_like(turned)
                    )
            gate[at, :] = dot(v, gw[...]).astype(BF16)

        def relay(i):
            for d in range(1, n_x):
                k = ((xi + d) % n_x) * 2 + core
                lat_copy(k, i, d, k).wait_recv()
                c = relay_copy(k, i, d)
                c.start()
                sends.append(c)

        l_ctx.wait()
        X[seq:block, :] = (ctx[...].astype(F32) * scale1 + shift1).astype(BF16)
        own_copy(partner).wait_recv()
        modulate(xi)
        l_ld.wait()
        l_rd.wait()
        encode(pl.ds(seq, ctx_rows), False)
        encode(chip_at(xi), True)
        relay(0)
        l_qd.wait()
        for c in l_q:
            c.wait()
        l_gw.wait()
        queries(xi)
        relay(1)
        for d in range(1, n_x):
            x2 = (xi + d) % n_x
            for i in range(2):
                relay_copy(x2 * 2 + 1 - core, i, d).wait_recv()
            modulate(x2)
            encode(chip_at(x2), True)

        right = ring_sp((r + 1) % n_sp, n_sp)
        left = ring_sp((r + n_sp - 1) % n_sp, n_sp)

        def part(owner, c):
            return codes.at[owner, pl.ds(pl.multiple_of(c * half, 16), half), :]

        def right_copy(owner, s):
            return remote(part(owner, core), part(owner, core), rr_s.at[s], rr_r.at[s], (right, tp))

        def left_copy(owner, s):
            return remote(part(owner, core), part(owner, core), rl_s.at[s], rl_r.at[s], (left, tp))

        def hand_right(owner, s, c):
            return remote(part(owner, c), part(owner, c), dr_s.at[s], dr_r.at[s], (sp, partner))

        def hand_left(owner, s, c):
            return remote(part(owner, c), part(owner, c), dl_s.at[s], dl_r.at[s], (sp, partner))

        right_copy(r, 1).start()
        left_copy(r, 1).start()

        for d in range(1, n_x):
            queries((xi + d) % n_x)

        for h in range(heads):
            M[h] = jnp.full((seq, LANES), -1e30, F32)
            O[h] = jnp.zeros((seq, LANES), F32)
        for c in l_kv:
            c.wait()

        def attend(owners, at, first, stop):
            cds = [codes[w, :, 0:lat_w] for w in owners]
            rts = [codes[w, :, lat_w : lat_w + LANES] for w in owners]

            def wide(v):
                whole, rest = block // LANES, block % LANES
                return jnp.concatenate([v] * whole + ([v[:, :rest]] if rest else []), axis=1)

            def one_pair(p, carry):
                kvs = [dot(cd, kv[p]).astype(BF16) for cd in cds]
                kcs = [jnp.concatenate([x[:, 0:LANES], rt], axis=1) for x, rt in zip(kvs, rts)]
                ln = lane_iota((block, LANES))
                ss = [
                    [
                        lax.dot_general(
                            Q[2 * p + e, at, :], kc, (((1,), (1,)), ((), ())), preferred_element_type=F32
                        )
                        for kc in kcs
                    ]
                    for e in range(2)
                ]
                for e in range(2):
                    h = 2 * p + e
                    top = M[h, at, :]
                    new = top
                    for s in ss[e]:
                        new = jnp.maximum(new, jnp.max(s, axis=1, keepdims=True))
                    M[h, at, :] = new
                    acc = O[h, at, :] * jnp.exp2(top - new)
                    for s, x in zip(ss[e], kvs):
                        w = jnp.exp2(s - wide(new)).astype(BF16)
                        v = x[:, LANES : 2 * LANES]
                        v = jnp.where((ln // HEAD) == e, v, jnp.ones_like(v))
                        acc = acc + dot(w, v)
                    O[h, at, :] = acc
                return carry

            lax.fori_loop(first, stop, one_pair, 0, unroll=min(2, stop - first))

        everything = pl.ds(0, seq)
        attend((r,), everything, 0, pairs)

        def arrive(s):
            from_left = (r + n_sp - s) % n_sp
            from_right = (r + s) % n_sp
            right_copy(from_left, s).wait_recv()
            right_copy(from_left, s + 1).start()
            hand_right(from_left, s, core).start()
            left_copy(from_right, s).wait_recv()

            @pl.when(s < last - 1)
            def _():
                left_copy(from_right, s + 1).start()

            hand_left(from_right, s, core).start()

        def near_blocks(s):
            from_left = (r + n_sp - s) % n_sp
            from_right = (r + s) % n_sp
            hand_right(from_left, s, 1 - core).wait_recv()
            hand_left(from_right, s, 1 - core).wait_recv()
            return from_left, from_right

        middle = pairs // 2

        def step(s, carry):
            near = near_blocks(s)
            attend(near, everything, 0, middle)
            arrive(s + 1)
            attend(near, everything, middle, pairs)
            return carry

        def finish(x):
            at = chip_at(x)
            ln2 = lane_iota((chip_rows, LANES))
            for p in range(pairs):
                a, b = O[2 * p, at, :], O[2 * p + 1, at, :]
                num = jnp.where(ln2 < HEAD, a, b)
                den = pltpu.roll(jnp.where(ln2 < HEAD, b, a), HEAD, 1)
                gt = gate[at, p * LANES : (p + 1) * LANES].astype(F32)
                gated[at, p * LANES : (p + 1) * LANES] = (num / den * silu(gt)).astype(BF16)

        arrive(1)
        lax.fori_loop(1, last - 1, step, 0)
        near = near_blocks(last - 1)
        others = [(xi + d) % n_x for d in range(1, n_x)]
        for x2 in others:
            attend(near, chip_at(x2), 0, middle)
        far = (r + n_sp - last) % n_sp
        right_copy(far, last).wait_recv()
        hand_right(far, last, core).start()
        for x2 in others:
            attend(near, chip_at(x2), middle, pairs)
        hand_right(far, last, 1 - core).wait_recv()
        l_ow.wait()

        def branch(t):
            return dot(gated[pl.ds(pl.multiple_of(t * rows, 8), rows), :], ow[...])

        def pair_copy(d):
            return remote(
                pair_out.at[d - 1], pair_in.at[d - 1], pr_s.at[d - 1], pr_r.at[d - 1], (sp, partner)
            )

        def over_chip(d):
            x2 = (xi + d) % n_x
            finish(x2)
            pair_out[d - 1] = branch(x2 * 2 + 1 - core).astype(BF16)
            c = pair_copy(d)
            c.start()
            sends.append(c)
            mine = branch(x2 * 2 + core)
            pair_copy(d).wait_recv()
            return mine + pair_in[d - 1].astype(F32)

        for d in range(1, n_x):
            x2 = (xi + d) % n_x
            attend((far,), chip_at(x2), 0, pairs)
            x_out[d - 1] = over_chip(d).astype(BF16)
            c = remote(x_out.at[d - 1], x_in.at[d - 1], xs_s.at[d - 1], xs_r.at[d - 1], (sp, x2 * 2 + core))
            c.start()
            sends.append(c)
        attend(near + (far,), chip_at(xi), 0, pairs)
        own_acc[...] = over_chip(n_x)
        acc = own_acc[...]
        for d in range(1, n_x):
            x2 = (xi + d) % n_x
            remote(
                x_out.at[d - 1], x_in.at[d - 1], xs_s.at[d - 1], xs_r.at[d - 1], (sp, x2 * 2 + core)
            ).wait_recv()
            acc = acc + x_in[d - 1].astype(F32)
        blended = residual_weight * lat[tp].astype(F32) + vec_row(4) * acc
        centred = blended - jnp.mean(blended, axis=-1, keepdims=True)
        var = jnp.mean(centred * centred, axis=-1, keepdims=True)
        out[...] = (centred * lax.rsqrt(var + norm_floor) * n_gain[...] + n_bias[...]).astype(BF16)

        for c in sends:
            c.wait_send()
        right_copy(r, 1).wait_send()
        left_copy(r, 1).wait_send()

        def drain(s, carry):
            right_copy(r, s + 1).wait_send()
            hand_right(r, s, core).wait_send()
            hand_left(r, s, core).wait_send()

            @pl.when(s < last - 1)
            def _():
                left_copy(r, s + 1).wait_send()

            return carry

        lax.fori_loop(1, last, drain, 0)
        hand_right(r, last, core).wait_send()

    def scratch():
        bf = lambda *s: pltpu.VMEM(s, BF16)
        f3 = lambda *s: pltpu.VMEM(s, F32)
        sem = lambda k: pltpu.SemaphoreType.DMA((k,))
        slab = width // n_sp
        return bf, f3, sem, slab

    return kernel, scratch, seq, block


def per_device(
    latents, context, cond_vec, ctx_vec, shift_w, scale_w, modgate_w, query_down_weight,
    latent_down_weight, rot_down, gate_w, query_norm_gain, latent_norm_gain, query_plain_weight,
    query_rotary_weight, key_expand_weight, value_expand_weight, out_w, norm_gain, norm_bias,
):
    n_sp, n_tp = lax.axis_size("sp"), lax.axis_size("tp")
    rows, width = latents.shape
    ctx_rows = context.shape[0]
    hcols = gate_w.shape[1]
    heads = hcols // HEAD
    slab = shift_w.shape[0]
    kernel, scratch, seq, block = make_kernel(n_sp, n_tp, rows, ctx_rows, width, heads)
    bf, f3, sem, _ = scratch()
    n_x = n_tp // 2
    last = n_sp // 2
    lat_w = latent_down_weight.shape[1]
    any_spec = pl.BlockSpec(memory_space=pl.ANY)
    vm = pl.BlockSpec(memory_space=pltpu.VMEM)
    call = pl.pallas_call(
        kernel,
        out_shape=jax.ShapeDtypeStruct((rows, width), BF16),
        in_specs=[any_spec] * 2 + [vm] * 2 + [any_spec] * 7 + [vm] * 2 + [any_spec] * 5 + [vm] * 2,
        out_specs=vm,
        scratch_shapes=[
            bf(n_tp, rows, width), bf(*context.shape), bf(*shift_w.shape), bf(*scale_w.shape),
            bf(*modgate_w.shape), bf(*query_down_weight.shape), bf(*latent_down_weight.shape),
            bf(*rot_down.shape[::-1]), bf(*gate_w.shape), bf(*query_plain_weight.shape),
            bf(*query_rotary_weight.shape), bf(heads // 2, lat_w, 2 * LANES), bf(*out_w.shape),
            f3(n_sp, 8, width // n_tp), f3(n_tp, 8, width // n_tp), bf(block, width),
            f3(seq, LANES), f3(seq, LANES), bf(n_sp, block, lat_w + LANES),
            bf(heads, seq, 2 * LANES), bf(seq, hcols), f3(heads, seq, LANES), f3(heads, seq, LANES),
            bf(seq, hcols), bf(n_x, rows, width), bf(n_x, rows, width), bf(n_x, rows, width),
            bf(n_x, rows, width), f3(rows, width),
            sem(12 + heads), sem(n_sp), sem(n_sp), sem(n_tp), sem(n_tp), sem(2 * n_x), sem(2 * n_tp), sem(2 * n_x), sem(2 * n_tp), sem(1), sem(1),
            sem(last + 1), sem(last + 1), sem(last + 1), sem(last + 1),
            sem(last + 1), sem(last + 1), sem(last + 1), sem(last + 1),
            sem(n_x), sem(n_x), sem(n_x), sem(n_x),
        ],
        compiler_params=pltpu.CompilerParams(
            collective_id=0, has_side_effects=True, vmem_limit_bytes=62 * 1024 * 1024
        ),
    )
    return call(
        latents, context, cond_vec.reshape(1, -1), ctx_vec.reshape(1, -1), shift_w, scale_w, modgate_w, query_down_weight,
        latent_down_weight, rot_down.T, gate_w, query_norm_gain.reshape(1, -1),
        latent_norm_gain.reshape(1, -1), query_plain_weight, query_rotary_weight,
        key_expand_weight, value_expand_weight, out_w, norm_gain.reshape(1, -1),
        norm_bias.reshape(1, -1),
    )


def solution(mesh):
    in_specs = (
        P(("sp", "tp"), None), P("sp", None), P(), P(), P("sp", "tp"), P("sp", "tp"), P("sp", "tp"),
        P(), P(), P(), P(None, "tp"), P(), P(), P(None, "tp"), P(None, "tp"), P(None, "tp"),
        P(None, "tp"), P("tp", None), P(), P(),
    )
    return jax.shard_map(
        per_device, mesh=mesh, in_specs=in_specs, out_specs=P(("sp", "tp"), None), check_vma=False
    )
```

```python
import math

import jax
import jax.numpy as jnp
from jax import lax
from jax.experimental import pallas as pl
from jax.experimental.pallas import tpu as pltpu
from jax.sharding import PartitionSpec as P

HEAD = 64
ROT = 32
GRID_W = 64
LANES = 128

rope_base = 10000.0
norm_floor = 1e-06
residual_weight = 2.0**0.5
F32 = jnp.float32
BF16 = jnp.bfloat16
MESH = pl.DeviceIdType.MESH


def dot(a, b):
    return jnp.dot(a, b, preferred_element_type=F32)


def ring_pos(sp, n):
    return jnp.where(sp % 2 == 0, sp // 2, n - 1 - sp // 2)


def ring_sp(r, n):
    return jnp.where(r < n // 2, 2 * r, 2 * (n - 1 - r) + 1)


def lane_iota(shape):
    return lax.broadcasted_iota(jnp.int32, shape, len(shape) - 1)


def make_kernel(n_sp, n_tp, rows, ctx_rows, width, heads):
    seq = rows * n_tp
    block = seq + ctx_rows
    half = block // 2
    n_x = n_tp // 2
    pairs = heads // 2
    q_groups = (heads * ROT) // LANES
    mod_cols = width // n_tp
    score_scale = (HEAD + ROT) ** (-0.5) * math.log2(math.e)
    last = n_sp // 2

    def kernel(
        lat_hbm, ctx_hbm, cond0, cond1, shift_hbm, scale_hbm, mgate_hbm, qd_hbm, ld_hbm, rd_hbm, gw_hbm,
        q_gain, l_gain, qp_hbm, qr_hbm, ke_hbm, ve_hbm, ow_hbm, n_gain, n_bias,
        out,
        lat, ctx, w_shift, w_scale, w_mgate, qd, ld, rd, gw, qp, qr, kv, ow,
        modbuf, vecs, X, cosb, sinb, codes, Q, gate, M, O, gated, pair_out, pair_in, x_out, x_in,
        own_acc,
        ld_sem, mod_s, mod_r, vec_s, vec_r, lat_s, lat_r, rel_s, rel_r, own_s, own_r,
        rr_s, rr_r, rl_s, rl_r, dr_s, dr_r, dl_s, dl_r, pr_s, pr_r, xs_s, xs_r,
    ):
        sp = lax.axis_index("sp")
        tp = lax.axis_index("tp")
        core = tp % 2
        xi = tp // 2
        partner = xi * 2 + (1 - core)
        r = ring_pos(sp, n_sp)

        loads = []

        def load(src, dst):
            c = pltpu.make_async_copy(src, dst, ld_sem.at[len(loads)])
            c.start()
            loads.append(c)
            return c

        l_mod = [load(shift_hbm, w_shift), load(scale_hbm, w_scale), load(mgate_hbm, w_mgate)]
        l_lat = load(lat_hbm, lat.at[tp])
        l_ctx = load(ctx_hbm, ctx)
        l_ld = load(ld_hbm, ld)
        l_rd = load(rd_hbm, rd)
        l_qd = load(qd_hbm, qd)
        l_gw = load(gw_hbm, gw)
        l_q = [load(qp_hbm, qp), load(qr_hbm, qr)]
        l_kv = []
        for p in range(pairs):
            cols = pl.ds(p * LANES, LANES)
            l_kv.append(load(ke_hbm.at[:, cols], kv.at[p, :, pl.ds(0, LANES)]))
            l_kv.append(load(ve_hbm.at[:, cols], kv.at[p, :, pl.ds(LANES, LANES)]))
        l_ow = load(ow_hbm, ow)

        bar = pltpu.get_barrier_semaphore()
        for d in range(1, n_sp):
            pl.semaphore_signal(bar, inc=1, device_id=((sp + d) % n_sp, tp), device_id_type=MESH)
        for d in range(1, n_tp):
            pl.semaphore_signal(bar, inc=1, device_id=(sp, (tp + d) % n_tp), device_id_type=MESH)

        for c in l_mod:
            c.wait()
        modbuf[sp] = jnp.zeros((8, mod_cols), F32)
        slab = w_shift.shape[0]

        def slab_of(ref):
            if slab % LANES == 0:
                return ref[:, pl.ds(pl.multiple_of(sp * slab, LANES), slab)]
            per = LANES // slab
            window = ref[:, pl.ds(pl.multiple_of(sp // per * LANES, LANES), LANES)]
            v = window[:, 0:slab]
            for i in range(1, per):
                v = jnp.where(sp % per == i, window[:, i * slab : (i + 1) * slab], v)
            return v

        def silu(v):
            return v / (1.0 + jnp.exp(-v))

        row_no = lax.broadcasted_iota(jnp.int32, (16, slab), 0)
        cv = jnp.where(row_no == 0, silu(slab_of(cond0)), silu(slab_of(cond1))).astype(BF16)
        for i, w in enumerate((w_shift, w_scale, w_mgate)):
            modbuf[sp, 2 * i : 2 * i + 2, :] = dot(cv, w[...])[0:2]
        pl.semaphore_wait(bar, n_sp + n_tp - 2)

        def remote(src, dst, s, rcv, dev):
            return pltpu.make_async_remote_copy(
                src_ref=src, dst_ref=dst, send_sem=s, recv_sem=rcv, device_id=dev, device_id_type=MESH
            )

        sends = []
        for d in range(1, n_sp):
            k = (sp + d) % n_sp
            c = remote(modbuf.at[sp], modbuf.at[sp], mod_s.at[d], mod_r.at[sp], (k, tp))
            c.start()
            sends.append(c)
        l_lat.wait()
        early = rows // 2 // 16 * 16
        pieces = (pl.ds(0, early), pl.ds(early, rows - early))

        def lat_copy(owner, i, d, k):
            return remote(
                lat.at[owner, pieces[i]], lat.at[owner, pieces[i]], lat_s.at[2 * d + i],
                lat_r.at[2 * owner + i], (sp, k),
            )

        def relay_copy(owner, i, d):
            return remote(
                lat.at[owner, pieces[i]], lat.at[owner, pieces[i]], rel_s.at[2 * d + i],
                rel_r.at[2 * owner + i], (sp, partner),
            )

        def own_copy(owner):
            return remote(lat.at[owner], lat.at[owner], own_s.at[0], own_r.at[0], (sp, partner))

        def send_piece(i):
            for d in range(1, n_x):
                c = lat_copy(tp, i, d, ((xi + d) % n_x) * 2 + core)
                c.start()
                sends.append(c)

        send_piece(0)
        c = own_copy(tp)
        c.start()
        sends.append(c)

        lane = lane_iota((seq, LANES))
        pos = sp * seq + lax.broadcasted_iota(jnp.int32, (seq, LANES), 0)
        pair_no = (lane % 8).astype(F32)
        inv = jnp.exp(pair_no * (-math.log(rope_base) / 8))
        grid_row = pos // GRID_W
        grid_col = pos - grid_row * GRID_W
        where_axis = jnp.where((lane % 32) < 16, grid_row, grid_col).astype(F32)
        ang = where_axis * inv
        cosb[...] = jnp.cos(ang)
        sinb[...] = jnp.where((lane % 16) < 8, -jnp.sin(ang), jnp.sin(ang))

        def rotate(v, at):
            ln = lane_iota(v.shape)
            sw = jnp.where((ln % 16) < 8, pltpu.roll(v, LANES - 8, 1), pltpu.roll(v, 8, 1))
            return v * cosb[at, :] + sw * sinb[at, :]

        for d in range(1, n_sp):
            k = (sp + d) % n_sp
            remote(modbuf.at[k], modbuf.at[k], mod_s.at[d], mod_r.at[k], (k, tp)).wait_recv()
        tot = modbuf[0]
        for k in range(1, n_sp):
            tot = tot + modbuf[k]
        vecs[tp] = tot
        for d in range(1, n_tp):
            k = (tp + d) % n_tp
            c = remote(vecs.at[tp], vecs.at[tp], vec_s.at[d], vec_r.at[tp], (sp, k))
            c.start()
            sends.append(c)
        send_piece(1)
        for d in range(1, n_tp):
            k = (tp + d) % n_tp
            remote(vecs.at[k], vecs.at[k], vec_s.at[d], vec_r.at[k], (sp, k)).wait_recv()

        def vec_row(i):
            return jnp.concatenate([vecs[t, i : i + 1, :] for t in range(n_tp)], axis=1)

        shift0, shift1 = vec_row(0), vec_row(1)
        scale0, scale1 = 1.0 + vec_row(2), 1.0 + vec_row(3)
        chip_rows = 2 * rows
        lat_w = ld.shape[1]

        def rms(v, g):
            return v * lax.rsqrt(jnp.mean(v * v, axis=-1, keepdims=True) + norm_floor) * g

        def chip_at(x):
            return pl.ds(pl.multiple_of(x * chip_rows, 16), chip_rows)

        def encode(at, turn):
            v = X[at, :]
            codes[r, at, 0:lat_w] = rms(dot(v, ld[...]), l_gain[...]).astype(BF16)
            kr = lax.dot_general(v, rd[...], (((1,), (1,)), ((), ())), preferred_element_type=F32)
            kr = jnp.concatenate([kr] * (LANES // ROT), axis=1)
            codes[r, at, lat_w : lat_w + LANES] = (rotate(kr, at) if turn else kr).astype(BF16)

        def modulate(x):
            for c in range(2):
                t = 2 * x + c
                X[pl.ds(pl.multiple_of(t * rows, 8), rows), :] = (
                    lat[t].astype(F32) * scale0 + shift0
                ).astype(BF16)

        def queries(x):
            at = chip_at(x)
            v = X[at, :]
            qc = rms(dot(v, qd[...]), q_gain[...]).astype(BF16)
            q_plain = (dot(qc, qp[...]) * score_scale).astype(BF16)
            q_rotary = dot(qc, qr[...]) * score_scale
            lane_q = lane_iota((chip_rows, LANES))
            for g in range(q_groups):
                turned = rotate(q_rotary[:, g * LANES : (g + 1) * LANES], at).astype(BF16)
                for i in range(LANES // ROT):
                    h = g * (LANES // ROT) + i
                    lo = (h // 2) * LANES
                    plain = q_plain[:, lo : lo + LANES]
                    Q[h, at, 0:LANES] = jnp.where((lane_q // HEAD) == h % 2, plain, jnp.zeros_like(plain))
                    Q[h, at, LANES : 2 * LANES] = jnp.where(
                        (lane_q // ROT) == i, turned, jnp.zeros_like(turned)
                    )
            gate[at, :] = dot(v, gw[...]).astype(BF16)

        def relay(i):
            for d in range(1, n_x):
                k = ((xi + d) % n_x) * 2 + core
                lat_copy(k, i, d, k).wait_recv()
                c = relay_copy(k, i, d)
                c.start()
                sends.append(c)

        l_ctx.wait()
        X[seq:block, :] = (ctx[...].astype(F32) * scale1 + shift1).astype(BF16)
        own_copy(partner).wait_recv()
        modulate(xi)
        l_ld.wait()
        l_rd.wait()
        encode(pl.ds(seq, ctx_rows), False)
        encode(chip_at(xi), True)
        relay(0)
        l_qd.wait()
        for c in l_q:
            c.wait()
        l_gw.wait()
        queries(xi)
        relay(1)
        for d in range(1, n_x):
            x2 = (xi + d) % n_x
            for i in range(2):
                relay_copy(x2 * 2 + 1 - core, i, d).wait_recv()
            modulate(x2)
            encode(chip_at(x2), True)

        right = ring_sp((r + 1) % n_sp, n_sp)
        left = ring_sp((r + n_sp - 1) % n_sp, n_sp)

        def part(owner, c):
            return codes.at[owner, pl.ds(pl.multiple_of(c * half, 16), half), :]

        def right_copy(owner, s):
            return remote(part(owner, core), part(owner, core), rr_s.at[s], rr_r.at[s], (right, tp))

        def left_copy(owner, s):
            return remote(part(owner, core), part(owner, core), rl_s.at[s], rl_r.at[s], (left, tp))

        first_rows = half // 2 // 16 * 16

        def end_right(owner):
            at = pl.ds(pl.multiple_of(core * half, 16), first_rows)
            return remote(
                codes.at[owner, at, :], codes.at[owner, at, :], rr_s.at[last], rr_r.at[last], (right, tp)
            )

        def end_left(owner):
            at = pl.ds(pl.multiple_of(core * half + first_rows, 16), half - first_rows)
            return remote(
                codes.at[owner, at, :], codes.at[owner, at, :], rl_s.at[last], rl_r.at[last], (left, tp)
            )

        def hand_right(owner, s, c):
            return remote(part(owner, c), part(owner, c), dr_s.at[s], dr_r.at[s], (sp, partner))

        def hand_left(owner, s, c):
            return remote(part(owner, c), part(owner, c), dl_s.at[s], dl_r.at[s], (sp, partner))

        right_copy(r, 1).start()
        left_copy(r, 1).start()

        for d in range(1, n_x):
            queries((xi + d) % n_x)

        for h in range(heads):
            M[h] = jnp.full((seq, LANES), -1e30, F32)
            O[h] = jnp.zeros((seq, LANES), F32)
        for c in l_kv:
            c.wait()

        def attend(owners, at, first, stop):
            cds = [codes[w, :, 0:lat_w] for w in owners]
            rts = [codes[w, :, lat_w : lat_w + LANES] for w in owners]

            def wide(v):
                whole, rest = block // LANES, block % LANES
                return jnp.concatenate([v] * whole + ([v[:, :rest]] if rest else []), axis=1)

            def one_pair(p, carry):
                kvs = [dot(cd, kv[p]).astype(BF16) for cd in cds]
                kcs = [jnp.concatenate([x[:, 0:LANES], rt], axis=1) for x, rt in zip(kvs, rts)]
                ln = lane_iota((block, LANES))
                ss = [
                    [
                        lax.dot_general(
                            Q[2 * p + e, at, :], kc, (((1,), (1,)), ((), ())), preferred_element_type=F32
                        )
                        for kc in kcs
                    ]
                    for e in range(2)
                ]
                for e in range(2):
                    h = 2 * p + e
                    top = M[h, at, :]
                    new = top
                    for s in ss[e]:
                        new = jnp.maximum(new, jnp.max(s, axis=1, keepdims=True))
                    M[h, at, :] = new
                    acc = O[h, at, :] * jnp.exp2(top - new)
                    for s, x in zip(ss[e], kvs):
                        w = jnp.exp2(s - wide(new)).astype(BF16)
                        v = x[:, LANES : 2 * LANES]
                        v = jnp.where((ln // HEAD) == e, v, jnp.ones_like(v))
                        acc = acc + dot(w, v)
                    O[h, at, :] = acc
                return carry

            lax.fori_loop(first, stop, one_pair, 0, unroll=min(2, stop - first))

        everything = pl.ds(0, seq)
        attend((r,), everything, 0, pairs)

        def arrive(s):
            from_left = (r + n_sp - s) % n_sp
            from_right = (r + s) % n_sp
            right_copy(from_left, s).wait_recv()

            @pl.when(s < last - 1)
            def _():
                right_copy(from_left, s + 1).start()

            @pl.when(s == last - 1)
            def _():
                end_right(from_left).start()

            left_copy(from_right, s).wait_recv()

            @pl.when(s < last - 1)
            def _():
                left_copy(from_right, s + 1).start()

            @pl.when(s == last - 1)
            def _():
                end_left(from_right).start()

            hand_right(from_left, s, core).start()
            hand_left(from_right, s, core).start()

        def near_blocks(s):
            from_left = (r + n_sp - s) % n_sp
            from_right = (r + s) % n_sp
            hand_right(from_left, s, 1 - core).wait_recv()
            hand_left(from_right, s, 1 - core).wait_recv()
            return from_left, from_right

        middle = pairs // 2

        def step(s, carry):
            near = near_blocks(s)
            attend(near, everything, 0, middle)
            arrive(s + 1)
            attend(near, everything, middle, pairs)
            return carry

        def finish(x):
            at = chip_at(x)
            ln2 = lane_iota((chip_rows, LANES))
            for p in range(pairs):
                a, b = O[2 * p, at, :], O[2 * p + 1, at, :]
                num = jnp.where(ln2 < HEAD, a, b)
                den = pltpu.roll(jnp.where(ln2 < HEAD, b, a), HEAD, 1)
                gt = gate[at, p * LANES : (p + 1) * LANES].astype(F32)
                gated[at, p * LANES : (p + 1) * LANES] = (num / den * silu(gt)).astype(BF16)

        arrive(1)
        lax.fori_loop(1, last - 1, step, 0)
        near = near_blocks(last - 1)
        others = [(xi + d) % n_x for d in range(1, n_x)]
        for x2 in others:
            attend(near, chip_at(x2), 0, middle)
        far = (r + n_sp - last) % n_sp
        end_right(far).wait_recv()
        end_left(far).wait_recv()
        hand_right(far, last, core).start()
        for x2 in others:
            attend(near, chip_at(x2), middle, pairs)
        hand_right(far, last, 1 - core).wait_recv()
        l_ow.wait()

        def branch(t):
            return dot(gated[pl.ds(pl.multiple_of(t * rows, 8), rows), :], ow[...])

        def pair_copy(d):
            return remote(
                pair_out.at[d - 1], pair_in.at[d - 1], pr_s.at[d - 1], pr_r.at[d - 1], (sp, partner)
            )

        def over_chip(d):
            x2 = (xi + d) % n_x
            finish(x2)
            pair_out[d - 1] = branch(x2 * 2 + 1 - core).astype(BF16)
            c = pair_copy(d)
            c.start()
            sends.append(c)
            mine = branch(x2 * 2 + core)
            pair_copy(d).wait_recv()
            return mine + pair_in[d - 1].astype(F32)

        for d in range(1, n_x):
            x2 = (xi + d) % n_x
            attend((far,), chip_at(x2), 0, pairs)
            x_out[d - 1] = over_chip(d).astype(BF16)
            c = remote(x_out.at[d - 1], x_in.at[d - 1], xs_s.at[d - 1], xs_r.at[d - 1], (sp, x2 * 2 + core))
            c.start()
            sends.append(c)
        attend(near + (far,), chip_at(xi), 0, pairs)
        own_acc[...] = over_chip(n_x)
        acc = own_acc[...]
        for d in range(1, n_x):
            x2 = (xi + d) % n_x
            remote(
                x_out.at[d - 1], x_in.at[d - 1], xs_s.at[d - 1], xs_r.at[d - 1], (sp, x2 * 2 + core)
            ).wait_recv()
            acc = acc + x_in[d - 1].astype(F32)
        blended = residual_weight * lat[tp].astype(F32) + vec_row(4) * acc
        centred = blended - jnp.mean(blended, axis=-1, keepdims=True)
        var = jnp.mean(centred * centred, axis=-1, keepdims=True)
        out[...] = (centred * lax.rsqrt(var + norm_floor) * n_gain[...] + n_bias[...]).astype(BF16)

        for c in sends:
            c.wait_send()
        right_copy(r, 1).wait_send()
        left_copy(r, 1).wait_send()

        def drain(s, carry):
            hand_right(r, s, core).wait_send()
            hand_left(r, s, core).wait_send()

            @pl.when(s < last - 1)
            def _():
                right_copy(r, s + 1).wait_send()
                left_copy(r, s + 1).wait_send()

            return carry

        lax.fori_loop(1, last, drain, 0)
        end_right(r).wait_send()
        end_left(r).wait_send()
        hand_right(r, last, core).wait_send()

    def scratch():
        bf = lambda *s: pltpu.VMEM(s, BF16)
        f3 = lambda *s: pltpu.VMEM(s, F32)
        sem = lambda k: pltpu.SemaphoreType.DMA((k,))
        slab = width // n_sp
        return bf, f3, sem, slab

    return kernel, scratch, seq, block


def per_device(
    latents, context, cond_vec, ctx_vec, shift_w, scale_w, modgate_w, query_down_weight,
    latent_down_weight, rot_down, gate_w, query_norm_gain, latent_norm_gain, query_plain_weight,
    query_rotary_weight, key_expand_weight, value_expand_weight, out_w, norm_gain, norm_bias,
):
    n_sp, n_tp = lax.axis_size("sp"), lax.axis_size("tp")
    rows, width = latents.shape
    ctx_rows = context.shape[0]
    hcols = gate_w.shape[1]
    heads = hcols // HEAD
    slab = shift_w.shape[0]
    kernel, scratch, seq, block = make_kernel(n_sp, n_tp, rows, ctx_rows, width, heads)
    bf, f3, sem, _ = scratch()
    n_x = n_tp // 2
    last = n_sp // 2
    lat_w = latent_down_weight.shape[1]
    any_spec = pl.BlockSpec(memory_space=pl.ANY)
    vm = pl.BlockSpec(memory_space=pltpu.VMEM)
    call = pl.pallas_call(
        kernel,
        out_shape=jax.ShapeDtypeStruct((rows, width), BF16),
        in_specs=[any_spec] * 2 + [vm] * 2 + [any_spec] * 7 + [vm] * 2 + [any_spec] * 5 + [vm] * 2,
        out_specs=vm,
        scratch_shapes=[
            bf(n_tp, rows, width), bf(*context.shape), bf(*shift_w.shape), bf(*scale_w.shape),
            bf(*modgate_w.shape), bf(*query_down_weight.shape), bf(*latent_down_weight.shape),
            bf(*rot_down.shape[::-1]), bf(*gate_w.shape), bf(*query_plain_weight.shape),
            bf(*query_rotary_weight.shape), bf(heads // 2, lat_w, 2 * LANES), bf(*out_w.shape),
            f3(n_sp, 8, width // n_tp), f3(n_tp, 8, width // n_tp), bf(block, width),
            f3(seq, LANES), f3(seq, LANES), bf(n_sp, block, lat_w + LANES),
            bf(heads, seq, 2 * LANES), bf(seq, hcols), f3(heads, seq, LANES), f3(heads, seq, LANES),
            bf(seq, hcols), bf(n_x, rows, width), bf(n_x, rows, width), bf(n_x, rows, width),
            bf(n_x, rows, width), f3(rows, width),
            sem(12 + heads), sem(n_sp), sem(n_sp), sem(n_tp), sem(n_tp), sem(2 * n_x), sem(2 * n_tp), sem(2 * n_x), sem(2 * n_tp), sem(1), sem(1),
            sem(last + 1), sem(last + 1), sem(last + 1), sem(last + 1),
            sem(last + 1), sem(last + 1), sem(last + 1), sem(last + 1),
            sem(n_x), sem(n_x), sem(n_x), sem(n_x),
        ],
        compiler_params=pltpu.CompilerParams(
            collective_id=0, has_side_effects=True, vmem_limit_bytes=62 * 1024 * 1024
        ),
    )
    return call(
        latents, context, cond_vec.reshape(1, -1), ctx_vec.reshape(1, -1), shift_w, scale_w, modgate_w, query_down_weight,
        latent_down_weight, rot_down.T, gate_w, query_norm_gain.reshape(1, -1),
        latent_norm_gain.reshape(1, -1), query_plain_weight, query_rotary_weight,
        key_expand_weight, value_expand_weight, out_w, norm_gain.reshape(1, -1),
        norm_bias.reshape(1, -1),
    )


def solution(mesh):
    in_specs = (
        P(("sp", "tp"), None), P("sp", None), P(), P(), P("sp", "tp"), P("sp", "tp"), P("sp", "tp"),
        P(), P(), P(), P(None, "tp"), P(), P(), P(None, "tp"), P(None, "tp"), P(None, "tp"),
        P(None, "tp"), P("tp", None), P(), P(),
    )
    return jax.shard_map(
        per_device, mesh=mesh, in_specs=in_specs, out_specs=P(("sp", "tp"), None), check_vma=False
    )
```
